32 devices in a mesh: grp: 2 (over y), sp: 4 (over z), tp: 4 (over x, core).
Axes of the slice: x: 2, y: 2, z: 4, core: 2. Of those that a mesh axis runs over, the one named last changes fastest.
Arguments:
- target: bfloat16 [2048, 2048], P(('grp', 'sp', 'tp')), parts along dimension 0, may hold values from -20 to 20
- source: bfloat16 [4096, 2048], P(('grp', 'sp')), parts along dimension 0, may hold values from -20 to 20
- source_gain: float32 [2048], replicated, may hold values from 0.1 to 1.9
- query_gain: float32 [2, 2048], replicated, may hold values from 0.1 to 1.9
- out_gain: float32 [2, 2048], replicated, may hold values from 0.1 to 1.9
- query_weight: bfloat16 [2, 2048, 2048], P(None, None, 'tp'), may hold values from -1 to 1
- key_weight: bfloat16 [2, 2048, 512], P(None, None, 'tp'), may hold values from -1 to 1
- value_weight: bfloat16 [2, 2048, 512], P(None, None, 'tp'), may hold values from -0.125 to 0.125
- out_weight: bfloat16 [2, 2048, 2048], P(None, 'tp'), may hold values from -0.125 to 0.125
Outputs:
- result: bfloat16 [2048, 2048], P(('grp', 'sp', 'tp')), parts along dimension 0
The draws below stay inside these ranges and needn't reach their ends.
There are 2 independent parts, one for each index of `grp`. The reference program is written for one: setup_inputs(seed, part) draws one part's arguments, and reference() takes and returns one part's arrays. A program takes and returns all parts, laid end to end along the dimension named above; an argument that names none is the same for every part. Nothing has to cross between parts.
All inputs are finite; a program needn't handle non-finite values.
Results may differ from the reference program's by a relative error of at most 0.024.
Values may be sent and summed in bfloat16 or wider, within the bound.
A program may use at most 64 MiB of HBM per device.

```python
import jax
import jax.numpy as jnp
from jax import lax

D = 2048
HD = 256
QH = 8
KVH = 2
LAYERS = 2
QW = 2048
KVW = 512
SRC = 2048
TGT = 1024


def feature_rows(key, row_count):
    keys_split = jax.random.split(key, 3)
    return jax.random.truncated_normal(keys_split[2], -5.0, 5.0, (row_count, D), jnp.float32)


def drawn_weight(key, fan_rows, columns):
    return jax.random.truncated_normal(key, -5.0, 5.0, (LAYERS, fan_rows, columns), jnp.float32) * fan_rows ** (-0.5)


def draw_target(key, part):
    own_key = jax.random.fold_in(key, 101)
    return feature_rows(own_key, TGT).astype(jnp.bfloat16)


def draw_source(key, part):
    own_key = jax.random.fold_in(key, 202)
    return feature_rows(own_key, SRC).astype(jnp.bfloat16)


def draw_query_weight(key, part):
    own_key = jax.random.fold_in(key, 303)
    return drawn_weight(own_key, D, QW).astype(jnp.bfloat16)


def draw_key_weight(key, part):
    own_key = jax.random.fold_in(key, 404)
    return drawn_weight(own_key, D, KVW).astype(jnp.bfloat16)


def level_of(stream_key, extent, cuts, low, top_value):
    level, own = 1.0, jax.random.fold_in(stream_key, 6)
    for dim, shards_of in cuts:
        heights = jnp.exp(jax.random.uniform(jax.random.fold_in(own, dim), (shards_of,), jnp.float32, low / len(cuts), top_value / len(cuts)))
        level = level * jnp.repeat(heights, extent[dim] // shards_of).reshape([-1 if axis == dim else 1 for axis in range(len(extent))])
    return level


def gaussian(stream_key, shape, spread, bound, pieces=(), kind=jnp.bfloat16):
    level = level_of(stream_key, shape, pieces, -0.22, 0.18) if pieces else 1.0
    drawn = jax.random.normal(stream_key, shape, jnp.float32) * spread * level
    return jnp.minimum(jnp.maximum(drawn, -bound), bound).astype(kind)


def setup_inputs(seed: int = 0, part: int = 0) -> dict:
    arg_keys = jax.random.split(jax.random.key(seed), 10)
    own_keys = jax.random.split(jax.random.fold_in(arg_keys[9], part), 10)
    return {
        "target": draw_target(jax.random.fold_in(jax.random.fold_in(arg_keys[9], part), 71), part),
        "source": draw_source(jax.random.fold_in(jax.random.fold_in(arg_keys[9], part), 71), part),
        "source_gain": jnp.clip(1.0 + 0.18 * jax.random.normal(arg_keys[2], (D,), jnp.float32), 0.1, 1.9),
        "query_gain": jnp.clip(1.0 + 0.18 * jax.random.normal(arg_keys[3], (LAYERS, D), jnp.float32), 0.1, 1.9),
        "out_gain": jnp.clip(1.0 + 0.18 * jax.random.normal(arg_keys[4], (LAYERS, D), jnp.float32), 0.1, 1.9),
        "query_weight": draw_query_weight(jax.random.fold_in(arg_keys[9], 71), part),
        "key_weight": draw_key_weight(jax.random.fold_in(arg_keys[9], 71), part),
        "value_weight": gaussian(arg_keys[7], (LAYERS, D, KVW), D ** -0.5, 0.125, ((2, 4),)),
        "out_weight": gaussian(arg_keys[8], (LAYERS, QW, D), QW ** -0.5, 0.125, ((1, 4),)),
    }


EPSILON = 1e-06

def rms_scaled(matrix_rows, gain_row):
    values = matrix_rows.astype(jnp.float32)
    inverse = lax.rsqrt(lax.optimization_barrier(jnp.mean(values * values, axis=-1, keepdims=True)) + EPSILON)
    return values * inverse * gain_row.astype(jnp.float32)

def reference(target, source, source_gain, query_gain, out_gain, query_weight, key_weight, value_weight, out_weight):
    normed_source = rms_scaled(source, source_gain).astype(jnp.bfloat16)
    heads_per_group = QH // KVH
    score_scale = HD ** (-0.5)
    residual = target
    for layer_index in range(LAYERS):
        all_keys = jnp.dot(normed_source, key_weight[layer_index], preferred_element_type=jnp.float32).astype(jnp.bfloat16)
        all_values = jnp.dot(normed_source, value_weight[layer_index], preferred_element_type=jnp.float32).astype(jnp.bfloat16)
        normed = rms_scaled(residual, query_gain[layer_index]).astype(jnp.bfloat16)
        queries = jnp.dot(normed, query_weight[layer_index], preferred_element_type=jnp.float32).astype(jnp.bfloat16)

        def one_head(head_index):
            key_head = head_index // heads_per_group
            query_rows = lax.dynamic_slice_in_dim(queries, head_index * HD, HD, 1)
            key_rows = lax.dynamic_slice_in_dim(all_keys, key_head * HD, HD, 1)
            value_rows = lax.dynamic_slice_in_dim(all_values, key_head * HD, HD, 1)
            scores = jnp.dot(query_rows, key_rows.T, preferred_element_type=jnp.float32) * score_scale
            row_peak = lax.optimization_barrier(jnp.max(scores, axis=1, keepdims=True))
            weights = jnp.exp(scores - row_peak)
            row_total = lax.optimization_barrier(jnp.sum(weights, axis=1, keepdims=True))
            mixed_rows = jnp.dot(weights.astype(jnp.bfloat16), value_rows, preferred_element_type=jnp.float32)
            return (mixed_rows / row_total).astype(jnp.bfloat16)
        head_outputs = lax.map(one_head, jnp.arange(QH, dtype=jnp.int32))
        attended = jnp.transpose(head_outputs, (1, 0, 2)).reshape(queries.shape[0], QH * HD)
        projected = jnp.dot(attended, out_weight[layer_index], preferred_element_type=jnp.float32)
        residual = (residual.astype(jnp.float32) + rms_scaled(projected, out_gain[layer_index])).astype(jnp.bfloat16)
    return residual
```

```python
import functools

import jax
import jax.numpy as jnp
from jax import lax
from jax.experimental import pallas as pl
from jax.experimental.pallas import tpu as pltpu
from jax.sharding import PartitionSpec as P

HD = 256
QH = 8
KVH = 2
LAYERS = 2


EPSILON = 1e-06


def swapped(value, axis, distance):
    mask = 2**distance
    pairs = [(source, source ^ mask) for source in range(lax.axis_size(axis))]
    return lax.ppermute(value, axis, pairs)


def rms_scaled(matrix_rows, gain_row):
    values = matrix_rows.astype(jnp.float32)
    inverse = lax.rsqrt(jnp.mean(values * values, axis=-1, keepdims=True) + EPSILON)
    return values * inverse * gain_row


def group_rounds(holding, bit_count, position):
    for bit_number in range(bit_count):
        my_bit = position >> bit_number & 1
        if holding.shape[0] > 1:
            halves = holding.reshape((holding.shape[0] // 2, 2) + holding.shape[1:])
            kept_part = lax.dynamic_index_in_dim(halves, my_bit, 1, False)
            outgoing = lax.dynamic_index_in_dim(halves, 1 - my_bit, 1, False)
        else:
            kept_part = holding
            outgoing = holding
        arrived = swapped(outgoing, "tp", bit_number)
        holding = jnp.where(
            my_bit == 0,
            jnp.concatenate([kept_part, arrived], 1),
            jnp.concatenate([arrived, kept_part], 1),
        )
    return holding


def spread_heads(factor, piece_index, piece_width):
    columns = jnp.repeat(factor, HD, axis=1)
    pieces = columns.reshape(factor.shape[0], columns.shape[1] // piece_width, piece_width)
    return jnp.take(pieces, piece_index, axis=1)


def merge_partials(weighted, row_peak, row_total, bit_count, position):
    piece_width = weighted.shape[2]
    piece_index = jnp.arange(weighted.shape[1], dtype=jnp.int32)
    for bit_number in range(bit_count):
        my_bit = position >> bit_number & 1
        halves = weighted.reshape(weighted.shape[0], weighted.shape[1] // 2, 2, piece_width)
        kept_part = lax.dynamic_index_in_dim(halves, my_bit, 2, False)
        outgoing = lax.dynamic_index_in_dim(halves, 1 - my_bit, 2, False)
        piece_index = lax.dynamic_index_in_dim(piece_index.reshape(-1, 2), my_bit, 1, False)
        far_weighted, far_peak, far_total = (
            swapped(outgoing.astype(jnp.bfloat16), "tp", bit_number).astype(outgoing.dtype),
            swapped(row_peak.astype(jnp.bfloat16), "tp", bit_number).astype(row_peak.dtype),
            swapped(row_total.astype(jnp.bfloat16), "tp", bit_number).astype(row_total.dtype),
        )
        new_peak = jnp.maximum(row_peak, far_peak)
        near_factor = jnp.exp(row_peak - new_peak)
        far_factor = jnp.exp(far_peak - new_peak)
        row_total = row_total * near_factor + far_total * far_factor
        weighted = kept_part * spread_heads(
            near_factor, piece_index, piece_width
        ) + far_weighted * spread_heads(far_factor, piece_index, piece_width)
        row_peak = new_peak
    return (weighted, row_total, piece_index)


def attend(carried, key_rows, value_rows, grouped, score_scale):
    row_peak, row_total, weighted = carried
    scores = (
        jnp.einsum("rhd,nd->rhn", grouped, key_rows, preferred_element_type=jnp.float32)
        * score_scale
    )
    new_peak = jnp.maximum(row_peak, jnp.max(scores, axis=2))
    weights = jnp.exp(scores - new_peak[:, :, None])
    row_total = jnp.sum(weights, axis=2)
    weighted = jnp.einsum(
        "rhn,nd->rhd", weights.astype(jnp.bfloat16), value_rows, preferred_element_type=jnp.float32
    )
    return (new_peak, row_total, weighted)


def body(
    target,
    source,
    source_gain,
    query_gain,
    out_gain,
    query_weight,
    key_weight,
    value_weight,
    out_weight,
):
    tp_devices = lax.axis_size("tp")
    group_size = tp_devices // KVH
    bit_count = group_size.bit_length() - 1
    position = lax.axis_index("tp") % group_size
    score_scale = HD ** (-0.5)
    heads_here = QH // KVH
    matrices = 2 * LAYERS
    slices = key_weight.shape[2]
    block_rows = source.shape[0] // group_size
    normed_source = rms_scaled(source, source_gain).astype(jnp.bfloat16)
    joined = jnp.concatenate(
        [
            matrix[layer_index]
            for layer_index in range(LAYERS)
            for matrix in (key_weight, value_weight)
        ],
        axis=1,
    )
    key_slices = jnp.dot(normed_source, joined, preferred_element_type=jnp.float32).astype(
        jnp.bfloat16
    )
    holding = group_rounds(
        key_slices.reshape(group_size, 1, block_rows, matrices, slices), bit_count, position
    )
    local_keys = jnp.transpose(holding[0], (2, 1, 0, 3)).reshape(matrices, block_rows, HD)
    residual = target
    stored = None
    for layer_index in range(LAYERS):
        normed = rms_scaled(residual, query_gain[layer_index]).astype(jnp.bfloat16)
        layer_weight = query_weight[layer_index]
        queries = jnp.dot(
            lax.all_gather(normed, "tp", axis=0, tiled=True),
            layer_weight,
            preferred_element_type=jnp.float32,
        ).astype(jnp.bfloat16)
        rows_all = queries.shape[0]
        gathered = group_rounds(queries[None, None], bit_count, position)[0]
        grouped = jnp.transpose(gathered, (1, 0, 2)).reshape(rows_all, heads_here, HD)
        start_state = (
            jnp.full((rows_all, heads_here), -1e30, jnp.float32),
            jnp.zeros((rows_all, heads_here), jnp.float32),
            jnp.zeros((rows_all, heads_here, HD), jnp.float32),
        )
        if layer_index == 0:
            empty_rows = jnp.zeros(
                (lax.axis_size("sp") * block_rows, matrices - 2, HD), jnp.bfloat16
            )
            later_keys = jnp.transpose(local_keys[2:], (1, 0, 2))
            updated = attend(
                (start_state + (empty_rows,))[:3],
                lax.all_gather(local_keys[0], "sp", axis=0, tiled=True),
                lax.all_gather(local_keys[1], "sp", axis=0, tiled=True),
                grouped,
                score_scale,
            )
            kept_rows = lax.all_gather(later_keys, "sp", axis=0, tiled=True)
            row_peak, row_total, weighted, stored = updated + (kept_rows,)
        else:
            row_peak, row_total, weighted = attend(
                start_state,
                stored[:, 2 * layer_index - 2],
                stored[:, 2 * layer_index - 1],
                grouped,
                score_scale,
            )
        piece_width = heads_here * HD // group_size
        merged, row_total, piece_index = merge_partials(
            weighted.reshape(rows_all, group_size, piece_width),
            row_peak,
            row_total,
            bit_count,
            position,
        )
        attended = (merged[:, 0] / spread_heads(row_total, piece_index, piece_width)[:, 0]).astype(
            jnp.bfloat16
        )
        out_layer = out_weight[layer_index]
        summed_rows = lax.psum_scatter(
            jnp.dot(attended, out_layer, preferred_element_type=jnp.float32).astype(jnp.bfloat16),
            "tp",
            scatter_dimension=0,
            tiled=True,
        ).astype(jnp.float32)
        residual = (
            residual.astype(jnp.float32) + rms_scaled(summed_rows, out_gain[layer_index])
        ).astype(jnp.bfloat16)
    return residual


CHUNKS = 4


def fused_kernel(
    n,
    target,
    source,
    source_gain,
    query_gain,
    out_gain,
    query_weight,
    key_weight,
    value_weight,
    out_weight,
    result,
    res,
    raw,
    ns,
    wkv,
    wq,
    wo,
    kh,
    xb,
    sb,
    rb,
    pj,
    qs,
    ms,
    ls,
    acc,
    load_sem,
    wload_sem,
    wsend,
    wrecv,
    xsend,
    xrecv,
    rsend,
    rrecv,
    zsend,
    zrecv,
    psend,
    precv,
):
    rows = target.shape[0]
    block = source.shape[0]
    half = key_weight.shape[2]
    wide = target.shape[1] // CHUNKS
    piece = block // CHUNKS
    heads = query_weight.shape[2] // HD
    z = lax.axis_index("sp")
    me = lax.axis_index("tp")
    c = me % 2
    partner = me + 1 - 2 * c
    across = (me + 2) % 4
    mesh_ids = pl.DeviceIdType.MESH
    f32, bf16 = jnp.float32, jnp.bfloat16

    loads = [pltpu.make_async_copy(target, res, load_sem.at[0])]
    for j in range(CHUNKS):
        part = pl.ds(j * piece, piece)
        loads.append(pltpu.make_async_copy(source.at[part], raw.at[part], load_sem.at[1 + j]))
    kv_loads, q_loads, o_loads = [], [], []
    for l in range(LAYERS):
        kv_loads.append(
            (
                pltpu.make_async_copy(key_weight.at[l], wkv.at[l, :, pl.ds(0, half)], wload_sem.at[l, 0]),
                pltpu.make_async_copy(value_weight.at[l], wkv.at[l, :, pl.ds(half, half)], wload_sem.at[l, 1]),
            )
        )
        q_loads.append(pltpu.make_async_copy(query_weight.at[l], wq.at[0, l], wload_sem.at[l, 2]))
        o_loads.append(pltpu.make_async_copy(out_weight.at[l], wo.at[0, l], wload_sem.at[l, 3]))
    for copy in loads:
        copy.start()
    for l in range(LAYERS):
        for copy in kv_loads[l]:
            copy.start()
    for l in range(LAYERS):
        q_loads[l].start()
        o_loads[l].start()

    def to_partner(src, dst, l, which):
        return pltpu.make_async_remote_copy(
            src_ref=src,
            dst_ref=dst,
            send_sem=wsend.at[l, which],
            recv_sem=wrecv.at[l, which],
            device_id={"tp": partner},
            device_id_type=mesh_ids,
        )

    q_share = [to_partner(query_weight.at[l], wq.at[1, l], l, 0) for l in range(LAYERS)]
    o_share = [to_partner(out_weight.at[l], wo.at[1, l], l, 1) for l in range(LAYERS)]

    def gather_copy(l, j):
        return pltpu.make_async_remote_copy(
            src_ref=xb.at[l, 0, j],
            dst_ref=xb.at[l, 1, j],
            send_sem=xsend.at[l, j],
            recv_sem=xrecv.at[l, j],
            device_id={"tp": across},
            device_id_type=mesh_ids,
        )

    def scatter_copy(l, j):
        return pltpu.make_async_remote_copy(
            src_ref=sb.at[l, j],
            dst_ref=rb.at[l, j],
            send_sem=rsend.at[l, j],
            recv_sem=rrecv.at[l, j],
            device_id={"tp": across},
            device_id_type=mesh_ids,
        )

    signs = (1, -1)

    def inside(index):
        return jnp.logical_and(index >= 0, index < n)

    def line_copy(l, way, d, kv):
        ref = kh.at[l, z - signs[way] * (d - 1), c, kv]
        return pltpu.make_async_remote_copy(
            src_ref=ref,
            dst_ref=ref,
            send_sem=zsend.at[l, way, d, kv],
            recv_sem=zrecv.at[l, way, d, kv],
            device_id={"sp": z + signs[way]},
            device_id_type=mesh_ids,
        )

    def line_arrival(l, way, d, kv):
        ref = kh.at[l, z - signs[way] * d, c, kv]
        return pltpu.make_async_remote_copy(
            src_ref=ref,
            dst_ref=ref,
            send_sem=zsend.at[l, way, d, kv],
            recv_sem=zrecv.at[l, way, d, kv],
            device_id={"sp": z - signs[way]},
            device_id_type=mesh_ids,
        )

    def pair_copy(l, way, d, kv, side):
        ref = kh.at[l, z - signs[way] * d, side, kv]
        return pltpu.make_async_remote_copy(
            src_ref=ref,
            dst_ref=ref,
            send_sem=psend.at[l, way, d, kv],
            recv_sem=precv.at[l, way, d, kv],
            device_id={"tp": partner},
            device_id_type=mesh_ids,
        )

    def send_own(l):
        for kv in range(2):
            for way in range(2):

                @pl.when(inside(z + signs[way]))
                def _():
                    line_copy(l, way, 1, kv).start()

            pair_copy(l, 0, 0, kv, c).start()

    def hand_on(l, d):
        for kv in range(2):
            for way in range(2):

                @pl.when(inside(z - signs[way] * d))
                def _():
                    line_arrival(l, way, d, kv).wait_recv()
                    if d < n - 1:

                        @pl.when(inside(z + signs[way]))
                        def _():
                            line_copy(l, way, d + 1, kv).start()

                    pair_copy(l, way, d, kv, c).start()

    def pair_arrivals(l):
        for kv in range(2):
            pair_copy(l, 0, 0, kv, 1 - c).wait_recv()
            for d in range(1, n):
                for way in range(2):

                    @pl.when(inside(z - signs[way] * d))
                    def _():
                        pair_copy(l, way, d, kv, 1 - c).wait_recv()

    def sends_done(l):
        for kv in range(2):
            pair_copy(l, 0, 0, kv, c).wait_send()
            for d in range(1, n):
                for way in range(2):

                    @pl.when(jnp.logical_and(inside(z - signs[way] * (d - 1)), inside(z + signs[way])))
                    def _():
                        line_copy(l, way, d, kv).wait_send()

                    @pl.when(inside(z - signs[way] * d))
                    def _():
                        pair_copy(l, way, d, kv, c).wait_send()

    barrier = pltpu.get_barrier_semaphore()
    pl.semaphore_signal(barrier, inc=1, device_id={"tp": partner}, device_id_type=mesh_ids)
    pl.semaphore_signal(barrier, inc=1, device_id={"tp": across}, device_id_type=mesh_ids)
    for d in range(1, n):
        pl.semaphore_signal(barrier, inc=1, device_id={"sp": (z + d) % n}, device_id_type=mesh_ids)
    pl.semaphore_wait(barrier, n + 1)
    q_share[0].start()

    def normed_rows(values, gain):
        inverse = lax.rsqrt(jnp.mean(values * values, axis=-1, keepdims=True) + EPSILON)
        return values * inverse * gain

    def share_normed(l):
        normed = normed_rows(res[...].astype(f32), query_gain[pl.ds(l, 1), :]).astype(bf16)
        for j in range(CHUNKS):
            xb[l, 0, j] = normed[:, j * wide : (j + 1) * wide]
            gather_copy(l, j).start()

    loads[0].wait()
    share_normed(0)

    for j in range(CHUNKS):
        loads[1 + j].wait()

    @pl.loop(0, block // 64)
    def _(i):
        part = pl.ds(pl.multiple_of(i * 64, 64), 64)
        ns[part, :] = normed_rows(raw[part, :].astype(f32), source_gain[...]).astype(bf16)

    for l in range(LAYERS):
        for copy in kv_loads[l]:
            copy.wait()
        made = jnp.dot(ns[...], wkv[l], preferred_element_type=f32).astype(bf16)
        kh[l, z, c, 0] = made[:, :half]
        kh[l, z, c, 1] = made[:, half:]
        if l == 0:
            send_own(0)
            o_share[0].start()

    def project_queries(l):
        q_loads[l].wait()
        q_share[l].wait_recv()
        mine = jnp.concatenate([xb[l, 0, j] for j in range(CHUNKS)], axis=1)
        for slot in range(2):
            made = jnp.dot(mine, wq[slot, l], preferred_element_type=f32).astype(bf16)
            for g in range(heads):
                qs[pl.ds((slot * heads + g) * 2 * rows, rows), :] = made[:, g * HD : (g + 1) * HD]
        if l == 1:
            hand_on(1, 2)
        totals = [None, None]
        for j in range(CHUNKS):
            gather_copy(l, j).wait_recv()
            for slot in range(2):
                made = jnp.dot(
                    xb[l, 1, j], wq[slot, l, pl.ds(j * wide, wide), :], preferred_element_type=f32
                )
                totals[slot] = made if j == 0 else totals[slot] + made
        for slot in range(2):
            made = totals[slot].astype(bf16)
            for g in range(heads):
                qs[pl.ds((slot * heads + g) * 2 * rows + rows, rows), :] = made[:, g * HD : (g + 1) * HD]

    def attend_all(l):
        ms[...] = jnp.full(ms.shape, -1e30, f32)
        ls[...] = jnp.zeros(ls.shape, f32)
        acc[...] = jnp.zeros(acc.shape, f32)

        @pl.loop(0, n)
        def _(s):
            keys = jnp.concatenate([kh[l, s, 0, 0], kh[l, s, 1, 0]], axis=1)
            values = jnp.concatenate([kh[l, s, 0, 1], kh[l, s, 1, 1]], axis=1)
            scores = lax.dot_general(
                qs[...], keys, (((1,), (1,)), ((), ())), preferred_element_type=f32
            ) * (HD ** (-0.5))
            old = ms[...]
            peak = jnp.maximum(old, jnp.max(scores, axis=1, keepdims=True))
            weights = jnp.exp(scores - peak)
            factor = jnp.exp(old - peak)
            ls[...] = ls[...] * factor + jnp.sum(weights, axis=1, keepdims=True)
            acc[...] = acc[...] * factor + jnp.dot(
                weights.astype(bf16), values, preferred_element_type=f32
            )
            ms[...] = peak

    for l in range(LAYERS):
        project_queries(l)
        if l == 0:
            hand_on(0, 1)
            for d in range(2, n):
                hand_on(0, d)
                if d == n - 2:
                    send_own(1)
        else:
            for d in range(3, n):
                hand_on(1, d)
        pair_arrivals(l)
        if l == 0:
            q_share[1].start()
            o_share[1].start()
        attend_all(l)
        out = (acc[...] / ls[...]).astype(bf16)
        lines = 2 * rows
        attended = [
            jnp.concatenate(
                [out[(slot * heads + g) * lines : (slot * heads + g + 1) * lines] for g in range(heads)], axis=1
            )
            for slot in range(2)
        ]
        o_loads[l].wait()
        o_share[l].wait_recv()
        for j in range(CHUNKS):
            cut = pl.ds(j * wide, wide)
            made = jnp.dot(attended[0], wo[0, l, :, cut], preferred_element_type=f32) + jnp.dot(
                attended[1], wo[1, l, :, cut], preferred_element_type=f32
            )
            sb[l, j] = made[rows:].astype(bf16)
            scatter_copy(l, j).start()
            pj[:, cut] = made[:rows]
        if l == 0:
            hand_on(1, 1)
        for j in range(CHUNKS):
            cut = pl.ds(j * wide, wide)
            scatter_copy(l, j).wait_recv()
            pj[:, cut] = pj[:, cut] + rb[l, j].astype(f32)
        res[...] = (
            res[...].astype(f32) + normed_rows(pj[...], out_gain[pl.ds(l, 1), :])
        ).astype(bf16)
        if l + 1 < LAYERS:
            share_normed(l + 1)
    result[...] = res[...]
    for l in range(LAYERS):
        q_share[l].wait_send()
        o_share[l].wait_send()
        for j in range(CHUNKS):
            gather_copy(l, j).wait_send()
            scatter_copy(l, j).wait_send()
        sends_done(l)


def fused_body(n, target, source, source_gain, query_gain, out_gain, query_weight, key_weight, value_weight, out_weight):
    rows, features = target.shape
    block = source.shape[0]
    half = key_weight.shape[2]
    columns = query_weight.shape[2]
    lines = 2 * rows * 2 * (columns // HD)
    wide = features // CHUNKS
    bf16, f32 = jnp.bfloat16, jnp.float32
    anywhere = pl.BlockSpec(memory_space=pl.ANY)
    inside = pl.BlockSpec(memory_space=pltpu.VMEM)
    dma = pltpu.SemaphoreType.DMA
    line = dma((LAYERS, 2, n, 2))
    return pl.pallas_call(
        functools.partial(fused_kernel, n),
        out_shape=jax.ShapeDtypeStruct(target.shape, bf16),
        in_specs=[anywhere, anywhere, inside, inside, inside, anywhere, anywhere, anywhere, anywhere],
        out_specs=inside,
        scratch_shapes=[
            pltpu.VMEM((rows, features), bf16),
            pltpu.VMEM((block, features), bf16),
            pltpu.VMEM((block, features), bf16),
            pltpu.VMEM((LAYERS, features, 2 * half), bf16),
            pltpu.VMEM((2, LAYERS, features, columns), bf16),
            pltpu.VMEM((2, LAYERS, columns, features), bf16),
            pltpu.VMEM((LAYERS, n, 2, 2, block, half), bf16),
            pltpu.VMEM((LAYERS, 2, CHUNKS, rows, wide), bf16),
            pltpu.VMEM((LAYERS, CHUNKS, rows, wide), bf16),
            pltpu.VMEM((LAYERS, CHUNKS, rows, wide), bf16),
            pltpu.VMEM((rows, features), f32),
            pltpu.VMEM((lines, HD), bf16),
            pltpu.VMEM((lines, 1), f32),
            pltpu.VMEM((lines, 1), f32),
            pltpu.VMEM((lines, HD), f32),
            dma((1 + CHUNKS,)),
            dma((LAYERS, 4)),
            dma((LAYERS, 2)),
            dma((LAYERS, 2)),
            dma((LAYERS, CHUNKS)),
            dma((LAYERS, CHUNKS)),
            dma((LAYERS, CHUNKS)),
            dma((LAYERS, CHUNKS)),
            line,
            line,
            line,
            line,
        ],
        compiler_params=pltpu.CompilerParams(
            collective_id=0, has_side_effects=True, vmem_limit_bytes=60 * 1024 * 1024
        ),
    )(
        target,
        source,
        source_gain[None],
        query_gain,
        out_gain,
        query_weight,
        key_weight,
        value_weight,
        out_weight,
    )


def solution(mesh):
    in_specs = (
        P(("grp", "sp", "tp"), None),
        P(("grp", "sp"), None),
        P(),
        P(),
        P(),
        P(None, None, "tp"),
        P(None, None, "tp"),
        P(None, None, "tp"),
        P(None, "tp", None),
    )
    out_specs = P(("grp", "sp", "tp"), None)
    chosen = body
    if mesh.shape["tp"] == 4 and KVH == 2 and LAYERS == 2 and mesh.shape["sp"] >= 4:
        chosen = functools.partial(fused_body, mesh.shape["sp"])
    return jax.shard_map(chosen, mesh=mesh, in_specs=in_specs, out_specs=out_specs, check_vma=False)
```

```python
import functools

import jax
import jax.numpy as jnp
from jax import lax
from jax.experimental import pallas as pl
from jax.experimental.pallas import tpu as pltpu
from jax.sharding import PartitionSpec as P

HD = 256
QH = 8
KVH = 2
LAYERS = 2


EPSILON = 1e-06
LOG2E = 1.4426950408889634


def swapped(value, axis, distance):
    mask = 2**distance
    pairs = [(source, source ^ mask) for source in range(lax.axis_size(axis))]
    return lax.ppermute(value, axis, pairs)


def rms_scaled(matrix_rows, gain_row):
    values = matrix_rows.astype(jnp.float32)
    inverse = lax.rsqrt(jnp.mean(values * values, axis=-1, keepdims=True) + EPSILON)
    return values * inverse * gain_row


def group_rounds(holding, bit_count, position):
    for bit_number in range(bit_count):
        my_bit = position >> bit_number & 1
        if holding.shape[0] > 1:
            halves = holding.reshape((holding.shape[0] // 2, 2) + holding.shape[1:])
            kept_part = lax.dynamic_index_in_dim(halves, my_bit, 1, False)
            outgoing = lax.dynamic_index_in_dim(halves, 1 - my_bit, 1, False)
        else:
            kept_part = holding
            outgoing = holding
        arrived = swapped(outgoing, "tp", bit_number)
        holding = jnp.where(
            my_bit == 0,
            jnp.concatenate([kept_part, arrived], 1),
            jnp.concatenate([arrived, kept_part], 1),
        )
    return holding


def spread_heads(factor, piece_index, piece_width):
    columns = jnp.repeat(factor, HD, axis=1)
    pieces = columns.reshape(factor.shape[0], columns.shape[1] // piece_width, piece_width)
    return jnp.take(pieces, piece_index, axis=1)


def merge_partials(weighted, row_peak, row_total, bit_count, position):
    piece_width = weighted.shape[2]
    piece_index = jnp.arange(weighted.shape[1], dtype=jnp.int32)
    for bit_number in range(bit_count):
        my_bit = position >> bit_number & 1
        halves = weighted.reshape(weighted.shape[0], weighted.shape[1] // 2, 2, piece_width)
        kept_part = lax.dynamic_index_in_dim(halves, my_bit, 2, False)
        outgoing = lax.dynamic_index_in_dim(halves, 1 - my_bit, 2, False)
        piece_index = lax.dynamic_index_in_dim(piece_index.reshape(-1, 2), my_bit, 1, False)
        far_weighted, far_peak, far_total = (
            swapped(outgoing.astype(jnp.bfloat16), "tp", bit_number).astype(outgoing.dtype),
            swapped(row_peak.astype(jnp.bfloat16), "tp", bit_number).astype(row_peak.dtype),
            swapped(row_total.astype(jnp.bfloat16), "tp", bit_number).astype(row_total.dtype),
        )
        new_peak = jnp.maximum(row_peak, far_peak)
        near_factor = jnp.exp(row_peak - new_peak)
        far_factor = jnp.exp(far_peak - new_peak)
        row_total = row_total * near_factor + far_total * far_factor
        weighted = kept_part * spread_heads(
            near_factor, piece_index, piece_width
        ) + far_weighted * spread_heads(far_factor, piece_index, piece_width)
        row_peak = new_peak
    return (weighted, row_total, piece_index)


def attend(carried, key_rows, value_rows, grouped, score_scale):
    row_peak, row_total, weighted = carried
    scores = (
        jnp.einsum("rhd,nd->rhn", grouped, key_rows, preferred_element_type=jnp.float32)
        * score_scale
    )
    new_peak = jnp.maximum(row_peak, jnp.max(scores, axis=2))
    weights = jnp.exp(scores - new_peak[:, :, None])
    row_total = jnp.sum(weights, axis=2)
    weighted = jnp.einsum(
        "rhn,nd->rhd", weights.astype(jnp.bfloat16), value_rows, preferred_element_type=jnp.float32
    )
    return (new_peak, row_total, weighted)


def body(
    target,
    source,
    source_gain,
    query_gain,
    out_gain,
    query_weight,
    key_weight,
    value_weight,
    out_weight,
):
    tp_devices = lax.axis_size("tp")
    group_size = tp_devices // KVH
    bit_count = group_size.bit_length() - 1
    position = lax.axis_index("tp") % group_size
    score_scale = HD ** (-0.5)
    heads_here = QH // KVH
    matrices = 2 * LAYERS
    slices = key_weight.shape[2]
    block_rows = source.shape[0] // group_size
    normed_source = rms_scaled(source, source_gain).astype(jnp.bfloat16)
    joined = jnp.concatenate(
        [
            matrix[layer_index]
            for layer_index in range(LAYERS)
            for matrix in (key_weight, value_weight)
        ],
        axis=1,
    )
    key_slices = jnp.dot(normed_source, joined, preferred_element_type=jnp.float32).astype(
        jnp.bfloat16
    )
    holding = group_rounds(
        key_slices.reshape(group_size, 1, block_rows, matrices, slices), bit_count, position
    )
    local_keys = jnp.transpose(holding[0], (2, 1, 0, 3)).reshape(matrices, block_rows, HD)
    residual = target
    stored = None
    for layer_index in range(LAYERS):
        normed = rms_scaled(residual, query_gain[layer_index]).astype(jnp.bfloat16)
        layer_weight = query_weight[layer_index]
        queries = jnp.dot(
            lax.all_gather(normed, "tp", axis=0, tiled=True),
            layer_weight,
            preferred_element_type=jnp.float32,
        ).astype(jnp.bfloat16)
        rows_all = queries.shape[0]
        gathered = group_rounds(queries[None, None], bit_count, position)[0]
        grouped = jnp.transpose(gathered, (1, 0, 2)).reshape(rows_all, heads_here, HD)
        start_state = (
            jnp.full((rows_all, heads_here), -1e30, jnp.float32),
            jnp.zeros((rows_all, heads_here), jnp.float32),
            jnp.zeros((rows_all, heads_here, HD), jnp.float32),
        )
        if layer_index == 0:
            empty_rows = jnp.zeros(
                (lax.axis_size("sp") * block_rows, matrices - 2, HD), jnp.bfloat16
            )
            later_keys = jnp.transpose(local_keys[2:], (1, 0, 2))
            updated = attend(
                (start_state + (empty_rows,))[:3],
                lax.all_gather(local_keys[0], "sp", axis=0, tiled=True),
                lax.all_gather(local_keys[1], "sp", axis=0, tiled=True),
                grouped,
                score_scale,
            )
            kept_rows = lax.all_gather(later_keys, "sp", axis=0, tiled=True)
            row_peak, row_total, weighted, stored = updated + (kept_rows,)
        else:
            row_peak, row_total, weighted = attend(
                start_state,
                stored[:, 2 * layer_index - 2],
                stored[:, 2 * layer_index - 1],
                grouped,
                score_scale,
            )
        piece_width = heads_here * HD // group_size
        merged, row_total, piece_index = merge_partials(
            weighted.reshape(rows_all, group_size, piece_width),
            row_peak,
            row_total,
            bit_count,
            position,
        )
        attended = (merged[:, 0] / spread_heads(row_total, piece_index, piece_width)[:, 0]).astype(
            jnp.bfloat16
        )
        out_layer = out_weight[layer_index]
        summed_rows = lax.psum_scatter(
            jnp.dot(attended, out_layer, preferred_element_type=jnp.float32).astype(jnp.bfloat16),
            "tp",
            scatter_dimension=0,
            tiled=True,
        ).astype(jnp.float32)
        residual = (
            residual.astype(jnp.float32) + rms_scaled(summed_rows, out_gain[layer_index])
        ).astype(jnp.bfloat16)
    return residual


CHUNKS = 4
PARTS = 2


def fused_kernel(
    n,
    target,
    source,
    source_gain,
    query_gain,
    out_gain,
    query_weight,
    key_weight,
    value_weight,
    out_weight,
    result,
    res,
    raw,
    ns,
    wkv,
    wq,
    wo,
    kh,
    xb,
    sb,
    rb,
    pj,
    qs,
    ms,
    ls,
    acc,
    load_sem,
    wload_sem,
    wsend,
    wrecv,
    xsend,
    xrecv,
    rsend,
    rrecv,
    zsend,
    zrecv,
    psend,
    precv,
):
    rows = target.shape[0]
    block = source.shape[0]
    half = key_weight.shape[2]
    wide = target.shape[1] // CHUNKS
    unit = block // PARTS
    lot = rows // PARTS
    heads = query_weight.shape[2] // HD
    z = lax.axis_index("sp")
    me = lax.axis_index("tp")
    c = me % 2
    partner = me + 1 - 2 * c
    across = (me + 2) % 4
    mesh_ids = pl.DeviceIdType.MESH
    f32, bf16 = jnp.float32, jnp.bfloat16

    loads = [pltpu.make_async_copy(target, res, load_sem.at[0])]
    for u in range(PARTS):
        part = pl.ds(u * unit, unit)
        loads.append(pltpu.make_async_copy(source.at[part], raw.at[part], load_sem.at[1 + u]))
    kv_loads, q_loads, o_loads = [], [], []
    for l in range(LAYERS):
        kv_loads.append(
            (
                pltpu.make_async_copy(key_weight.at[l], wkv.at[l, :, pl.ds(0, half)], wload_sem.at[l, 0]),
                pltpu.make_async_copy(value_weight.at[l], wkv.at[l, :, pl.ds(half, half)], wload_sem.at[l, 1]),
            )
        )
        q_loads.append(pltpu.make_async_copy(query_weight.at[l], wq.at[0, l], wload_sem.at[l, 2]))
        o_loads.append(pltpu.make_async_copy(out_weight.at[l], wo.at[0, l], wload_sem.at[l, 3]))
    for copy in loads:
        copy.start()
    for copy in kv_loads[0]:
        copy.start()

    def to_partner(src, dst, l, which):
        return pltpu.make_async_remote_copy(
            src_ref=src,
            dst_ref=dst,
            send_sem=wsend.at[l, which],
            recv_sem=wrecv.at[l, which],
            device_id={"tp": partner},
            device_id_type=mesh_ids,
        )

    q_share = [to_partner(query_weight.at[l], wq.at[1, l], l, 0) for l in range(LAYERS)]
    o_share = [to_partner(out_weight.at[l], wo.at[1, l], l, 1) for l in range(LAYERS)]

    def gather_copy(l, j):
        return pltpu.make_async_remote_copy(
            src_ref=xb.at[l, 0, j],
            dst_ref=xb.at[l, 1, j],
            send_sem=xsend.at[l, j],
            recv_sem=xrecv.at[l, j],
            device_id={"tp": across},
            device_id_type=mesh_ids,
        )

    def scatter_copy(l, j):
        return pltpu.make_async_remote_copy(
            src_ref=sb.at[l, j],
            dst_ref=rb.at[l, j],
            send_sem=rsend.at[l, j],
            recv_sem=rrecv.at[l, j],
            device_id={"tp": across},
            device_id_type=mesh_ids,
        )

    signs = (1, -1)

    def inside(index):
        return jnp.logical_and(index >= 0, index < n)

    def line_copy(l, way, d, u):
        ref = kh.at[l, z - signs[way] * (d - 1), c, u]
        return pltpu.make_async_remote_copy(
            src_ref=ref,
            dst_ref=ref,
            send_sem=zsend.at[l, way, d, u],
            recv_sem=zrecv.at[l, way, d, u],
            device_id={"sp": z + signs[way]},
            device_id_type=mesh_ids,
        )

    def line_arrival(l, way, d, u):
        ref = kh.at[l, z - signs[way] * d, c, u]
        return pltpu.make_async_remote_copy(
            src_ref=ref,
            dst_ref=ref,
            send_sem=zsend.at[l, way, d, u],
            recv_sem=zrecv.at[l, way, d, u],
            device_id={"sp": z - signs[way]},
            device_id_type=mesh_ids,
        )

    def pair_copy(l, way, d, u, side):
        ref = kh.at[l, z - signs[way] * d, side, u]
        return pltpu.make_async_remote_copy(
            src_ref=ref,
            dst_ref=ref,
            send_sem=psend.at[l, way, d, u],
            recv_sem=precv.at[l, way, d, u],
            device_id={"tp": partner},
            device_id_type=mesh_ids,
        )

    def send_own(l, u):
        for way in range(2):

            @pl.when(inside(z + signs[way]))
            def _():
                line_copy(l, way, 1, u).start()

        pair_copy(l, 0, 0, u, c).start()

    def hand_on(l, d):
        for u in range(PARTS):
            for way in range(2):

                @pl.when(inside(z - signs[way] * d))
                def _():
                    line_arrival(l, way, d, u).wait_recv()
                    if d < n - 1:

                        @pl.when(inside(z + signs[way]))
                        def _():
                            line_copy(l, way, d + 1, u).start()

                    pair_copy(l, way, d, u, c).start()

    def pair_arrivals(l, d):
        for u in range(PARTS):
            if d == 0:
                pair_copy(l, 0, 0, u, 1 - c).wait_recv()
                continue
            for way in range(2):

                @pl.when(inside(z - signs[way] * d))
                def _():
                    pair_copy(l, way, d, u, 1 - c).wait_recv()

    def sends_done(l):
        for u in range(PARTS):
            pair_copy(l, 0, 0, u, c).wait_send()
            for d in range(1, n):
                for way in range(2):

                    @pl.when(jnp.logical_and(inside(z - signs[way] * (d - 1)), inside(z + signs[way])))
                    def _():
                        line_copy(l, way, d, u).wait_send()

                    @pl.when(inside(z - signs[way] * d))
                    def _():
                        pair_copy(l, way, d, u, c).wait_send()

    barrier = pltpu.get_barrier_semaphore()
    pl.semaphore_signal(barrier, inc=1, device_id={"tp": partner}, device_id_type=mesh_ids)
    pl.semaphore_signal(barrier, inc=1, device_id={"tp": across}, device_id_type=mesh_ids)
    for d in range(1, n):
        pl.semaphore_signal(barrier, inc=1, device_id={"sp": (z + d) % n}, device_id_type=mesh_ids)
    pl.semaphore_wait(barrier, n + 1)
    def normed_rows(values, gain):
        inverse = lax.rsqrt(jnp.mean(values * values, axis=-1, keepdims=True) + EPSILON)
        return values * inverse * gain

    def share_normed(l, r):
        part = pl.ds(r * lot, lot)
        normed = normed_rows(res[part, :].astype(f32), query_gain[pl.ds(l, 1), :])
        xb[l, 0, r] = normed.astype(bf16)
        gather_copy(l, r).start()

    loads[0].wait()
    for r in range(PARTS):
        share_normed(0, r)

    def make_keys(l, u):
        made = jnp.dot(ns[pl.ds(u * unit, unit), :], wkv[l], preferred_element_type=f32).astype(bf16)
        kh[l, z, c, u, 0] = made[:, :half]
        kh[l, z, c, u, 1] = made[:, half:]

    for u in range(PARTS):
        loads[1 + u].wait()

        @pl.loop(0, unit // 64)
        def _(i):
            part = pl.ds(pl.multiple_of(u * unit + i * 64, 64), 64)
            ns[part, :] = normed_rows(raw[part, :].astype(f32), source_gain[...]).astype(bf16)

        if u == 0:
            for copy in kv_loads[0]:
                copy.wait()
        make_keys(0, u)
        send_own(0, u)
    q_loads[0].start()
    q_share[0].start()
    for copy in kv_loads[1]:
        copy.start()
    o_loads[0].start()
    o_share[0].start()
    q_loads[1].start()
    o_loads[1].start()

    band = 2 * heads * rows

    def project_queries(l, i):
        lines = jnp.concatenate([xb[l, i, r] for r in range(PARTS)], axis=0)
        for slot in range(2):
            made = jnp.dot(lines, wq[slot, l], preferred_element_type=f32).astype(bf16)
            for g in range(heads):
                qs[pl.ds(i * band + (slot * heads + g) * rows, rows), :] = made[:, g * HD : (g + 1) * HD]

    def attend(l, s, i, first):
        def joined(kv):
            return jnp.concatenate(
                [jnp.concatenate([kh[l, s, 0, u, kv], kh[l, s, 1, u, kv]], axis=1) for u in range(PARTS)], axis=0
            )

        part = pl.ds(i * band, band)
        scores = lax.dot_general(
            qs[part, :], joined(0), (((1,), (1,)), ((), ())), preferred_element_type=f32
        ) * (HD ** (-0.5) * LOG2E)
        peak = jnp.max(scores, axis=1, keepdims=True)
        if not first:
            old = ms[part, :]
            peak = jnp.maximum(old, peak)
            factor = jnp.exp2(old - peak)
        weights = jnp.exp2(scores - peak)
        sums = weights[:, :128]
        for k in range(128, block, 128):
            sums = sums + weights[:, k : k + 128]
        mixed = jnp.dot(weights.astype(bf16), joined(1), preferred_element_type=f32)
        ms[part, :] = peak
        if first:
            ls[part, :] = sums
            acc[part, :] = mixed
        else:
            ls[part, :] = ls[part, :] * factor + sums
            acc[part, :] = acc[part, :] * factor + mixed

    def attend_step(l, d, sides):
        if d == 0:
            for i in sides:
                attend(l, z, i, True)
            return

        @pl.loop(jnp.where(z - d >= 0, 0, 1), jnp.where(z + d < n, 2, 1))
        def _(way):
            for i in sides:
                attend(l, z - (1 - 2 * way) * d, i, False)

    def project_out(l, i):
        part = pl.ds(i * band, band)
        out = (acc[part, :] / jnp.sum(ls[part, :], axis=1, keepdims=True)).astype(bf16)
        attended = [
            jnp.concatenate(
                [out[(slot * heads + g) * rows : (slot * heads + g + 1) * rows] for g in range(heads)], axis=1
            )
            for slot in range(2)
        ]
        for j in range(CHUNKS):
            cut = pl.ds(j * wide, wide)
            made = jnp.dot(attended[0], wo[0, l, :, cut], preferred_element_type=f32) + jnp.dot(
                attended[1], wo[1, l, :, cut], preferred_element_type=f32
            )
            if i == 0:
                pj[:, cut] = made
            else:
                for r in range(PARTS):
                    sb[l, r, :, cut] = made[r * lot : (r + 1) * lot].astype(bf16)

    def finish(l, tail):
        project_out(l, 1)
        for r in range(PARTS):
            scatter_copy(l, r).start()
        tail()
        project_out(l, 0)
        for r in range(PARTS):
            part = pl.ds(r * lot, lot)
            scatter_copy(l, r).wait_recv()
            total = pj[part, :] + rb[l, r].astype(f32)
            res[part, :] = (
                res[part, :].astype(f32) + normed_rows(total, out_gain[pl.ds(l, 1), :])
            ).astype(bf16)
            if l + 1 < LAYERS:
                share_normed(l + 1, r)

    q_loads[0].wait()
    q_share[0].wait_recv()
    project_queries(0, 0)
    for copy in kv_loads[1]:
        copy.wait()
    for u in range(PARTS):
        make_keys(1, u)
    for r in range(PARTS):
        gather_copy(0, r).wait_recv()
    project_queries(0, 1)
    for d in range(1, n):
        hand_on(0, d)
        if d == n - 2:
            for u in range(PARTS):
                send_own(1, u)
        pair_arrivals(0, d - 1)
        attend_step(0, d - 1, (1, 0))
    pair_arrivals(0, n - 1)
    q_share[1].start()
    o_share[1].start()
    attend_step(0, n - 1, (1,))
    o_loads[0].wait()
    o_share[0].wait_recv()

    def tail_first():
        hand_on(1, 1)
        attend_step(0, n - 1, (0,))

    finish(0, tail_first)

    q_loads[1].wait()
    q_share[1].wait_recv()
    hand_on(1, 2)
    project_queries(1, 0)
    pair_arrivals(1, 0)
    attend_step(1, 0, (0,))
    pair_arrivals(1, 1)
    attend_step(1, 1, (0,))
    pair_arrivals(1, 2)
    attend_step(1, 2, (0,))
    for d in range(3, n):
        hand_on(1, d)
    for r in range(PARTS):
        gather_copy(1, r).wait_recv()
    project_queries(1, 1)
    for d in range(n):
        if d > 2:
            pair_arrivals(1, d)
        attend_step(1, d, (1,))
    o_loads[1].wait()
    o_share[1].wait_recv()

    def tail_second():
        for d in range(3, n):
            attend_step(1, d, (0,))

    finish(1, tail_second)
    result[...] = res[...]
    for l in range(LAYERS):
        q_share[l].wait_send()
        o_share[l].wait_send()
        for r in range(PARTS):
            gather_copy(l, r).wait_send()
            scatter_copy(l, r).wait_send()
        sends_done(l)


def fused_body(n, target, source, source_gain, query_gain, out_gain, query_weight, key_weight, value_weight, out_weight):
    rows, features = target.shape
    block = source.shape[0]
    half = key_weight.shape[2]
    columns = query_weight.shape[2]
    lines = 2 * rows * 2 * (columns // HD)
    lot = rows // PARTS
    bf16, f32 = jnp.bfloat16, jnp.float32
    anywhere = pl.BlockSpec(memory_space=pl.ANY)
    inside = pl.BlockSpec(memory_space=pltpu.VMEM)
    dma = pltpu.SemaphoreType.DMA
    line = dma((LAYERS, 2, n, PARTS))
    return pl.pallas_call(
        functools.partial(fused_kernel, n),
        out_shape=jax.ShapeDtypeStruct(target.shape, bf16),
        in_specs=[anywhere, anywhere, inside, inside, inside, anywhere, anywhere, anywhere, anywhere],
        out_specs=inside,
        scratch_shapes=[
            pltpu.VMEM((rows, features), bf16),
            pltpu.VMEM((block, features), bf16),
            pltpu.VMEM((block, features), bf16),
            pltpu.VMEM((LAYERS, features, 2 * half), bf16),
            pltpu.VMEM((2, LAYERS, features, columns), bf16),
            pltpu.VMEM((2, LAYERS, columns, features), bf16),
            pltpu.VMEM((LAYERS, n, 2, PARTS, 2, block // PARTS, half), bf16),
            pltpu.VMEM((LAYERS, 2, PARTS, lot, features), bf16),
            pltpu.VMEM((LAYERS, PARTS, lot, features), bf16),
            pltpu.VMEM((LAYERS, PARTS, lot, features), bf16),
            pltpu.VMEM((rows, features), f32),
            pltpu.VMEM((lines, HD), bf16),
            pltpu.VMEM((lines, 1), f32),
            pltpu.VMEM((lines, 128), f32),
            pltpu.VMEM((lines, HD), f32),
            dma((1 + PARTS,)),
            dma((LAYERS, 4)),
            dma((LAYERS, 2)),
            dma((LAYERS, 2)),
            dma((LAYERS, PARTS)),
            dma((LAYERS, PARTS)),
            dma((LAYERS, PARTS)),
            dma((LAYERS, PARTS)),
            line,
            line,
            line,
            line,
        ],
        compiler_params=pltpu.CompilerParams(
            collective_id=0, has_side_effects=True, vmem_limit_bytes=60 * 1024 * 1024
        ),
    )(
        target,
        source,
        source_gain[None],
        query_gain,
        out_gain,
        query_weight,
        key_weight,
        value_weight,
        out_weight,
    )


def solution(mesh):
    in_specs = (
        P(("grp", "sp", "tp"), None),
        P(("grp", "sp"), None),
        P(),
        P(),
        P(),
        P(None, None, "tp"),
        P(None, None, "tp"),
        P(None, None, "tp"),
        P(None, "tp", None),
    )
    out_specs = P(("grp", "sp", "tp"), None)
    chosen = body
    if mesh.shape["tp"] == 4 and KVH == 2 and LAYERS == 2 and mesh.shape["sp"] >= 4:
        chosen = functools.partial(fused_body, mesh.shape["sp"])
    return jax.shard_map(chosen, mesh=mesh, in_specs=in_specs, out_specs=out_specs, check_vma=False)
```

```python
import functools

import jax
import jax.numpy as jnp
from jax import lax
from jax.experimental import pallas as pl
from jax.experimental.pallas import tpu as pltpu
from jax.sharding import PartitionSpec as P

HD = 256
QH = 8
KVH = 2
LAYERS = 2


EPSILON = 1e-06
LOG2E = 1.4426950408889634


def swapped(value, axis, distance):
    mask = 2**distance
    pairs = [(source, source ^ mask) for source in range(lax.axis_size(axis))]
    return lax.ppermute(value, axis, pairs)


def rms_scaled(matrix_rows, gain_row):
    values = matrix_rows.astype(jnp.float32)
    inverse = lax.rsqrt(jnp.mean(values * values, axis=-1, keepdims=True) + EPSILON)
    return values * inverse * gain_row


def group_rounds(holding, bit_count, position):
    for bit_number in range(bit_count):
        my_bit = position >> bit_number & 1
        if holding.shape[0] > 1:
            halves = holding.reshape((holding.shape[0] // 2, 2) + holding.shape[1:])
            kept_part = lax.dynamic_index_in_dim(halves, my_bit, 1, False)
            outgoing = lax.dynamic_index_in_dim(halves, 1 - my_bit, 1, False)
        else:
            kept_part = holding
            outgoing = holding
        arrived = swapped(outgoing, "tp", bit_number)
        holding = jnp.where(
            my_bit == 0,
            jnp.concatenate([kept_part, arrived], 1),
            jnp.concatenate([arrived, kept_part], 1),
        )
    return holding


def spread_heads(factor, piece_index, piece_width):
    columns = jnp.repeat(factor, HD, axis=1)
    pieces = columns.reshape(factor.shape[0], columns.shape[1] // piece_width, piece_width)
    return jnp.take(pieces, piece_index, axis=1)


def merge_partials(weighted, row_peak, row_total, bit_count, position):
    piece_width = weighted.shape[2]
    piece_index = jnp.arange(weighted.shape[1], dtype=jnp.int32)
    for bit_number in range(bit_count):
        my_bit = position >> bit_number & 1
        halves = weighted.reshape(weighted.shape[0], weighted.shape[1] // 2, 2, piece_width)
        kept_part = lax.dynamic_index_in_dim(halves, my_bit, 2, False)
        outgoing = lax.dynamic_index_in_dim(halves, 1 - my_bit, 2, False)
        piece_index = lax.dynamic_index_in_dim(piece_index.reshape(-1, 2), my_bit, 1, False)
        far_weighted, far_peak, far_total = (
            swapped(outgoing.astype(jnp.bfloat16), "tp", bit_number).astype(outgoing.dtype),
            swapped(row_peak.astype(jnp.bfloat16), "tp", bit_number).astype(row_peak.dtype),
            swapped(row_total.astype(jnp.bfloat16), "tp", bit_number).astype(row_total.dtype),
        )
        new_peak = jnp.maximum(row_peak, far_peak)
        near_factor = jnp.exp(row_peak - new_peak)
        far_factor = jnp.exp(far_peak - new_peak)
        row_total = row_total * near_factor + far_total * far_factor
        weighted = kept_part * spread_heads(
            near_factor, piece_index, piece_width
        ) + far_weighted * spread_heads(far_factor, piece_index, piece_width)
        row_peak = new_peak
    return (weighted, row_total, piece_index)


def attend(carried, key_rows, value_rows, grouped, score_scale):
    row_peak, row_total, weighted = carried
    scores = (
        jnp.einsum("rhd,nd->rhn", grouped, key_rows, preferred_element_type=jnp.float32)
        * score_scale
    )
    new_peak = jnp.maximum(row_peak, jnp.max(scores, axis=2))
    weights = jnp.exp(scores - new_peak[:, :, None])
    row_total = jnp.sum(weights, axis=2)
    weighted = jnp.einsum(
        "rhn,nd->rhd", weights.astype(jnp.bfloat16), value_rows, preferred_element_type=jnp.float32
    )
    return (new_peak, row_total, weighted)


def body(
    target,
    source,
    source_gain,
    query_gain,
    out_gain,
    query_weight,
    key_weight,
    value_weight,
    out_weight,
):
    tp_devices = lax.axis_size("tp")
    group_size = tp_devices // KVH
    bit_count = group_size.bit_length() - 1
    position = lax.axis_index("tp") % group_size
    score_scale = HD ** (-0.5)
    heads_here = QH // KVH
    matrices = 2 * LAYERS
    slices = key_weight.shape[2]
    block_rows = source.shape[0] // group_size
    normed_source = rms_scaled(source, source_gain).astype(jnp.bfloat16)
    joined = jnp.concatenate(
        [
            matrix[layer_index]
            for layer_index in range(LAYERS)
            for matrix in (key_weight, value_weight)
        ],
        axis=1,
    )
    key_slices = jnp.dot(normed_source, joined, preferred_element_type=jnp.float32).astype(
        jnp.bfloat16
    )
    holding = group_rounds(
        key_slices.reshape(group_size, 1, block_rows, matrices, slices), bit_count, position
    )
    local_keys = jnp.transpose(holding[0], (2, 1, 0, 3)).reshape(matrices, block_rows, HD)
    residual = target
    stored = None
    for layer_index in range(LAYERS):
        normed = rms_scaled(residual, query_gain[layer_index]).astype(jnp.bfloat16)
        layer_weight = query_weight[layer_index]
        queries = jnp.dot(
            lax.all_gather(normed, "tp", axis=0, tiled=True),
            layer_weight,
            preferred_element_type=jnp.float32,
        ).astype(jnp.bfloat16)
        rows_all = queries.shape[0]
        gathered = group_rounds(queries[None, None], bit_count, position)[0]
        grouped = jnp.transpose(gathered, (1, 0, 2)).reshape(rows_all, heads_here, HD)
        start_state = (
            jnp.full((rows_all, heads_here), -1e30, jnp.float32),
            jnp.zeros((rows_all, heads_here), jnp.float32),
            jnp.zeros((rows_all, heads_here, HD), jnp.float32),
        )
        if layer_index == 0:
            empty_rows = jnp.zeros(
                (lax.axis_size("sp") * block_rows, matrices - 2, HD), jnp.bfloat16
            )
            later_keys = jnp.transpose(local_keys[2:], (1, 0, 2))
            updated = attend(
                (start_state + (empty_rows,))[:3],
                lax.all_gather(local_keys[0], "sp", axis=0, tiled=True),
                lax.all_gather(local_keys[1], "sp", axis=0, tiled=True),
                grouped,
                score_scale,
            )
            kept_rows = lax.all_gather(later_keys, "sp", axis=0, tiled=True)
            row_peak, row_total, weighted, stored = updated + (kept_rows,)
        else:
            row_peak, row_total, weighted = attend(
                start_state,
                stored[:, 2 * layer_index - 2],
                stored[:, 2 * layer_index - 1],
                grouped,
                score_scale,
            )
        piece_width = heads_here * HD // group_size
        merged, row_total, piece_index = merge_partials(
            weighted.reshape(rows_all, group_size, piece_width),
            row_peak,
            row_total,
            bit_count,
            position,
        )
        attended = (merged[:, 0] / spread_heads(row_total, piece_index, piece_width)[:, 0]).astype(
            jnp.bfloat16
        )
        out_layer = out_weight[layer_index]
        summed_rows = lax.psum_scatter(
            jnp.dot(attended, out_layer, preferred_element_type=jnp.float32).astype(jnp.bfloat16),
            "tp",
            scatter_dimension=0,
            tiled=True,
        ).astype(jnp.float32)
        residual = (
            residual.astype(jnp.float32) + rms_scaled(summed_rows, out_gain[layer_index])
        ).astype(jnp.bfloat16)
    return residual


CHUNKS = 4
PARTS = 2


def fused_kernel(
    n,
    target,
    source,
    source_gain,
    query_gain,
    out_gain,
    query_weight,
    key_weight,
    value_weight,
    out_weight,
    result,
    res,
    raw,
    ns,
    wkv,
    wq,
    wo,
    kh,
    xb,
    sb,
    rb,
    pj,
    qs,
    ms,
    ls,
    acc,
    load_sem,
    wload_sem,
    wsend,
    wrecv,
    xsend,
    xrecv,
    rsend,
    rrecv,
    zsend,
    zrecv,
    psend,
    precv,
):
    rows = target.shape[0]
    block = source.shape[0]
    half = key_weight.shape[2]
    wide = target.shape[1] // CHUNKS
    unit = block // PARTS
    lot = rows // PARTS
    heads = query_weight.shape[2] // HD
    z = lax.axis_index("sp")
    me = lax.axis_index("tp")
    c = me % 2
    partner = me + 1 - 2 * c
    across = (me + 2) % 4
    mesh_ids = pl.DeviceIdType.MESH
    f32, bf16 = jnp.float32, jnp.bfloat16

    loads = [pltpu.make_async_copy(target, res, load_sem.at[0])]
    for u in range(PARTS):
        part = pl.ds(u * unit, unit)
        loads.append(pltpu.make_async_copy(source.at[part], raw.at[part], load_sem.at[1 + u]))
    kv_loads, q_loads, o_loads = [], [], []
    for l in range(LAYERS):
        kv_loads.append(
            (
                pltpu.make_async_copy(key_weight.at[l], wkv.at[l, :, pl.ds(0, half)], wload_sem.at[l, 0]),
                pltpu.make_async_copy(value_weight.at[l], wkv.at[l, :, pl.ds(half, half)], wload_sem.at[l, 1]),
            )
        )
        q_loads.append(pltpu.make_async_copy(query_weight.at[l], wq.at[0, l], wload_sem.at[l, 2]))
        o_loads.append(pltpu.make_async_copy(out_weight.at[l], wo.at[0, l], wload_sem.at[l, 3]))
    for copy in loads:
        copy.start()
    for copy in kv_loads[0]:
        copy.start()

    def to_partner(src, dst, l, which):
        return pltpu.make_async_remote_copy(
            src_ref=src,
            dst_ref=dst,
            send_sem=wsend.at[l, which],
            recv_sem=wrecv.at[l, which],
            device_id={"tp": partner},
            device_id_type=mesh_ids,
        )

    q_share = [to_partner(query_weight.at[l], wq.at[1, l], l, 0) for l in range(LAYERS)]
    o_share = [to_partner(out_weight.at[l], wo.at[1, l], l, 1) for l in range(LAYERS)]

    def gather_copy(l, j):
        return pltpu.make_async_remote_copy(
            src_ref=xb.at[l, 0, j],
            dst_ref=xb.at[l, 1, j],
            send_sem=xsend.at[l, j],
            recv_sem=xrecv.at[l, j],
            device_id={"tp": across},
            device_id_type=mesh_ids,
        )

    def scatter_copy(l, j):
        return pltpu.make_async_remote_copy(
            src_ref=sb.at[l, j],
            dst_ref=rb.at[l, j],
            send_sem=rsend.at[l, j],
            recv_sem=rrecv.at[l, j],
            device_id={"tp": across},
            device_id_type=mesh_ids,
        )

    signs = (1, -1)

    def inside(index):
        return jnp.logical_and(index >= 0, index < n)

    def line_copy(l, way, d, u):
        ref = kh.at[l, z - signs[way] * (d - 1), c, u]
        return pltpu.make_async_remote_copy(
            src_ref=ref,
            dst_ref=ref,
            send_sem=zsend.at[l, way, d, u],
            recv_sem=zrecv.at[l, way, d, u],
            device_id={"sp": z + signs[way]},
            device_id_type=mesh_ids,
        )

    def line_arrival(l, way, d, u):
        ref = kh.at[l, z - signs[way] * d, c, u]
        return pltpu.make_async_remote_copy(
            src_ref=ref,
            dst_ref=ref,
            send_sem=zsend.at[l, way, d, u],
            recv_sem=zrecv.at[l, way, d, u],
            device_id={"sp": z - signs[way]},
            device_id_type=mesh_ids,
        )

    def pair_copy(l, way, d, u, side):
        ref = kh.at[l, z - signs[way] * d, side, u]
        return pltpu.make_async_remote_copy(
            src_ref=ref,
            dst_ref=ref,
            send_sem=psend.at[l, way, d, u],
            recv_sem=precv.at[l, way, d, u],
            device_id={"tp": partner},
            device_id_type=mesh_ids,
        )

    def send_own(l, u):
        for way in range(2):

            @pl.when(inside(z + signs[way]))
            def _():
                line_copy(l, way, 1, u).start()

        pair_copy(l, 0, 0, u, c).start()

    def hand_on(l, d, units=range(PARTS)):
        for u in units:
            for way in range(2):

                @pl.when(inside(z - signs[way] * d))
                def _():
                    line_arrival(l, way, d, u).wait_recv()
                    if d < n - 1:

                        @pl.when(inside(z + signs[way]))
                        def _():
                            line_copy(l, way, d + 1, u).start()

                    pair_copy(l, way, d, u, c).start()

    def pair_arrivals(l, d):
        for u in range(PARTS):
            if d == 0:
                pair_copy(l, 0, 0, u, 1 - c).wait_recv()
                continue
            for way in range(2):

                @pl.when(inside(z - signs[way] * d))
                def _():
                    pair_copy(l, way, d, u, 1 - c).wait_recv()

    def sends_done(l):
        for u in range(PARTS):
            pair_copy(l, 0, 0, u, c).wait_send()
            for d in range(1, n):
                for way in range(2):

                    @pl.when(jnp.logical_and(inside(z - signs[way] * (d - 1)), inside(z + signs[way])))
                    def _():
                        line_copy(l, way, d, u).wait_send()

                    @pl.when(inside(z - signs[way] * d))
                    def _():
                        pair_copy(l, way, d, u, c).wait_send()

    barrier = pltpu.get_barrier_semaphore()
    pl.semaphore_signal(barrier, inc=1, device_id={"tp": partner}, device_id_type=mesh_ids)
    pl.semaphore_signal(barrier, inc=1, device_id={"tp": across}, device_id_type=mesh_ids)
    for d in range(1, n):
        pl.semaphore_signal(barrier, inc=1, device_id={"sp": (z + d) % n}, device_id_type=mesh_ids)
    pl.semaphore_wait(barrier, n + 1)
    def normed_rows(values, gain):
        inverse = lax.rsqrt(jnp.mean(values * values, axis=-1, keepdims=True) + EPSILON)
        return values * inverse * gain

    def share_normed(l, r):
        part = pl.ds(r * lot, lot)
        normed = normed_rows(res[part, :].astype(f32), query_gain[pl.ds(l, 1), :])
        xb[l, 0, r] = normed.astype(bf16)
        gather_copy(l, r).start()

    def make_keys(l, u):
        made = jnp.dot(ns[pl.ds(u * unit, unit), :], wkv[l], preferred_element_type=f32).astype(bf16)
        kh[l, z, c, u, 0] = made[:, :half]
        kh[l, z, c, u, 1] = made[:, half:]

    for u in range(PARTS):
        loads[1 + u].wait()

        @pl.loop(0, unit // 64)
        def _(i):
            part = pl.ds(pl.multiple_of(u * unit + i * 64, 64), 64)
            ns[part, :] = normed_rows(raw[part, :].astype(f32), source_gain[...]).astype(bf16)

        if u == 0:
            for copy in kv_loads[0]:
                copy.wait()
            q_loads[0].start()
            for copy in kv_loads[1]:
                copy.start()
        make_keys(0, u)
        send_own(0, u)
        if u == 0:
            loads[0].wait()
            for r in range(PARTS):
                share_normed(0, r)
    q_share[0].start()
    o_loads[0].start()
    o_share[0].start()
    q_loads[1].start()
    o_loads[1].start()

    band = 2 * heads * rows

    def project_queries(l, i):
        lines = jnp.concatenate([xb[l, i, r] for r in range(PARTS)], axis=0)
        for slot in range(2):
            made = jnp.dot(lines, wq[slot, l], preferred_element_type=f32).astype(bf16)
            for g in range(heads):
                qs[pl.ds(i * band + (slot * heads + g) * rows, rows), :] = made[:, g * HD : (g + 1) * HD]

    def attend(l, s, i, first):
        def joined(kv):
            return jnp.concatenate(
                [jnp.concatenate([kh[l, s, 0, u, kv], kh[l, s, 1, u, kv]], axis=1) for u in range(PARTS)], axis=0
            )

        part = pl.ds(i * band, band)
        scores = lax.dot_general(
            qs[part, :], joined(0), (((1,), (1,)), ((), ())), preferred_element_type=f32
        ) * (HD ** (-0.5) * LOG2E)
        peak = jnp.max(scores, axis=1, keepdims=True)
        if not first:
            old = ms[part, :]
            peak = jnp.maximum(old, peak)
            factor = jnp.exp2(old - peak)
        weights = jnp.exp2(scores - peak)
        sums = weights[:, :128]
        for k in range(128, block, 128):
            sums = sums + weights[:, k : k + 128]
        mixed = jnp.dot(weights.astype(bf16), joined(1), preferred_element_type=f32)
        ms[part, :] = peak
        if first:
            ls[part, :] = sums
            acc[part, :] = mixed
        else:
            ls[part, :] = ls[part, :] * factor + sums
            acc[part, :] = acc[part, :] * factor + mixed

    def attend_step(l, d, sides):
        if d == 0:
            for i in sides:
                attend(l, z, i, True)
            return

        @pl.loop(jnp.where(z - d >= 0, 0, 1), jnp.where(z + d < n, 2, 1))
        def _(way):
            for i in sides:
                attend(l, z - (1 - 2 * way) * d, i, False)

    def project_out(l, i):
        part = pl.ds(i * band, band)
        out = (acc[part, :] / jnp.sum(ls[part, :], axis=1, keepdims=True)).astype(bf16)
        attended = [
            jnp.concatenate(
                [out[(slot * heads + g) * rows : (slot * heads + g + 1) * rows] for g in range(heads)], axis=1
            )
            for slot in range(2)
        ]
        for j in range(CHUNKS):
            cut = pl.ds(j * wide, wide)
            made = jnp.dot(attended[0], wo[0, l, :, cut], preferred_element_type=f32) + jnp.dot(
                attended[1], wo[1, l, :, cut], preferred_element_type=f32
            )
            if i == 0:
                pj[:, cut] = made
            else:
                for r in range(PARTS):
                    sb[l, r, :, cut] = made[r * lot : (r + 1) * lot].astype(bf16)

    def finish(l, tail):
        project_out(l, 1)
        for r in range(PARTS):
            scatter_copy(l, r).start()
        tail()
        project_out(l, 0)
        for r in range(PARTS):
            part = pl.ds(r * lot, lot)
            scatter_copy(l, r).wait_recv()
            total = pj[part, :] + rb[l, r].astype(f32)
            res[part, :] = (
                res[part, :].astype(f32) + normed_rows(total, out_gain[pl.ds(l, 1), :])
            ).astype(bf16)
            if l + 1 < LAYERS:
                share_normed(l + 1, r)

    for copy in kv_loads[1]:
        copy.wait()
    for u in range(PARTS):
        make_keys(1, u)
    hand_on(0, 1, (0,))
    q_loads[0].wait()
    q_share[0].wait_recv()
    project_queries(0, 0)
    hand_on(0, 1, (1,))
    for r in range(PARTS):
        gather_copy(0, r).wait_recv()
    project_queries(0, 1)
    for d in range(2, n):
        hand_on(0, d, (0,))
        pair_arrivals(0, d - 2)
        attend_step(0, d - 2, (1, 0))
        hand_on(0, d, (1,))
        if d == n - 2:
            for u in range(PARTS):
                send_own(1, u)
    pair_arrivals(0, n - 2)
    attend_step(0, n - 2, (1, 0))
    pair_arrivals(0, n - 1)
    q_share[1].start()
    o_share[1].start()
    attend_step(0, n - 1, (1,))
    o_loads[0].wait()
    o_share[0].wait_recv()

    def tail_first():
        hand_on(1, 1)
        attend_step(0, n - 1, (0,))

    finish(0, tail_first)

    q_loads[1].wait()
    q_share[1].wait_recv()
    hand_on(1, 2)
    project_queries(1, 0)
    pair_arrivals(1, 0)
    attend_step(1, 0, (0,))
    pair_arrivals(1, 1)
    attend_step(1, 1, (0,))
    pair_arrivals(1, 2)
    attend_step(1, 2, (0,))
    for d in range(3, n):
        hand_on(1, d)
    for r in range(PARTS):
        gather_copy(1, r).wait_recv()
    project_queries(1, 1)
    for d in range(n):
        if d > 2:
            pair_arrivals(1, d)
        attend_step(1, d, (1,))
    o_loads[1].wait()
    o_share[1].wait_recv()

    def tail_second():
        for d in range(3, n):
            attend_step(1, d, (0,))

    finish(1, tail_second)
    result[...] = res[...]
    for l in range(LAYERS):
        q_share[l].wait_send()
        o_share[l].wait_send()
        for r in range(PARTS):
            gather_copy(l, r).wait_send()
            scatter_copy(l, r).wait_send()
        sends_done(l)


def fused_body(n, target, source, source_gain, query_gain, out_gain, query_weight, key_weight, value_weight, out_weight):
    rows, features = target.shape
    block = source.shape[0]
    half = key_weight.shape[2]
    columns = query_weight.shape[2]
    lines = 2 * rows * 2 * (columns // HD)
    lot = rows // PARTS
    bf16, f32 = jnp.bfloat16, jnp.float32
    anywhere = pl.BlockSpec(memory_space=pl.ANY)
    inside = pl.BlockSpec(memory_space=pltpu.VMEM)
    dma = pltpu.SemaphoreType.DMA
    line = dma((LAYERS, 2, n, PARTS))
    return pl.pallas_call(
        functools.partial(fused_kernel, n),
        out_shape=jax.ShapeDtypeStruct(target.shape, bf16),
        in_specs=[anywhere, anywhere, inside, inside, inside, anywhere, anywhere, anywhere, anywhere],
        out_specs=inside,
        scratch_shapes=[
            pltpu.VMEM((rows, features), bf16),
            pltpu.VMEM((block, features), bf16),
            pltpu.VMEM((block, features), bf16),
            pltpu.VMEM((LAYERS, features, 2 * half), bf16),
            pltpu.VMEM((2, LAYERS, features, columns), bf16),
            pltpu.VMEM((2, LAYERS, columns, features), bf16),
            pltpu.VMEM((LAYERS, n, 2, PARTS, 2, block // PARTS, half), bf16),
            pltpu.VMEM((LAYERS, 2, PARTS, lot, features), bf16),
            pltpu.VMEM((LAYERS, PARTS, lot, features), bf16),
            pltpu.VMEM((LAYERS, PARTS, lot, features), bf16),
            pltpu.VMEM((rows, features), f32),
            pltpu.VMEM((lines, HD), bf16),
            pltpu.VMEM((lines, 1), f32),
            pltpu.VMEM((lines, 128), f32),
            pltpu.VMEM((lines, HD), f32),
            dma((1 + PARTS,)),
            dma((LAYERS, 4)),
            dma((LAYERS, 2)),
            dma((LAYERS, 2)),
            dma((LAYERS, PARTS)),
            dma((LAYERS, PARTS)),
            dma((LAYERS, PARTS)),
            dma((LAYERS, PARTS)),
            line,
            line,
            line,
            line,
        ],
        compiler_params=pltpu.CompilerParams(
            collective_id=0, has_side_effects=True, vmem_limit_bytes=60 * 1024 * 1024
        ),
    )(
        target,
        source,
        source_gain[None],
        query_gain,
        out_gain,
        query_weight,
        key_weight,
        value_weight,
        out_weight,
    )


def solution(mesh):
    in_specs = (
        P(("grp", "sp", "tp"), None),
        P(("grp", "sp"), None),
        P(),
        P(),
        P(),
        P(None, None, "tp"),
        P(None, None, "tp"),
        P(None, None, "tp"),
        P(None, "tp", None),
    )
    out_specs = P(("grp", "sp", "tp"), None)
    chosen = body
    if mesh.shape["tp"] == 4 and KVH == 2 and LAYERS == 2 and mesh.shape["sp"] >= 4:
        chosen = functools.partial(fused_body, mesh.shape["sp"])
    return jax.shard_map(chosen, mesh=mesh, in_specs=in_specs, out_specs=out_specs, check_vma=False)
```
